32 devices in a mesh: ep: 8 (over z, y), tp: 4 (over x, core).
Axes of the slice: x: 2, y: 2, z: 4, core: 2. Of those that a mesh axis runs over, the one named last changes fastest.
Arguments:
- tokens: bfloat16 [128, 2048], P('ep'), may hold values from -6 to 6
- norm_gain: bfloat16 [2048], replicated, may hold values from 0.099609375 to 1.8984375
- query_weight: bfloat16 [2048, 1024], P('ep', 'tp'), may hold values from -0.125 to 0.125
- key_weight: bfloat16 [2048, 1024], P('ep', 'tp'), may hold values from -0.125 to 0.125
- value_weight: bfloat16 [2048, 2048], P('ep', 'tp'), may hold values from -0.125 to 0.125
- outgate_weight: bfloat16 [2048, 2048], P('ep', 'tp'), may hold values from -0.125 to 0.125
- beta_weight: bfloat16 [2048, 16], replicated, may hold values from -0.125 to 0.125
- decay_weight: bfloat16 [2048, 16], replicated, may hold values from -0.125 to 0.125
- decay_rate: float32 [16], P('tp'), may hold values from 0.02 to 6
- decay_bias: float32 [16], P('tp'), may hold values from -3 to 3
- head_gain: bfloat16 [128], replicated, may hold values from 0.099609375 to 1.8984375
- recurrent: float32 [128, 16, 128, 128], P('ep', 'tp'), may hold values from -3 to 3
- output_weight: bfloat16 [2048, 2048], P('tp', 'ep'), may hold values from -0.125 to 0.125
- ffn_gain: bfloat16 [2048], replicated, may hold values from 0.099609375 to 1.8984375
- routes: int32 [128, 4], P('ep'), may hold values from 0 to 7, all different within a row; in each aligned block of 16 rows (0 to 15, 16 to 31, ...) at most 16 rows name the same one
- route_weight: float32 [128, 4], P('ep'), may hold values from 0.1 to 1
- expert_gate: bfloat16 [8, 2048, 512], P('ep', None, 'tp'), may hold values from -0.125 to 0.125
- expert_up: bfloat16 [8, 2048, 512], P('ep', None, 'tp'), may hold values from -0.125 to 0.125
- expert_down: bfloat16 [8, 512, 2048], P('ep', 'tp'), may hold values from -0.25 to 0.25
- shared_gate: bfloat16 [2048, 512], P('ep', 'tp'), may hold values from -0.125 to 0.125
- shared_up: bfloat16 [2048, 512], P('ep', 'tp'), may hold values from -0.125 to 0.125
- shared_down: bfloat16 [512, 2048], P('tp', 'ep'), may hold values from -0.25 to 0.25
- branch_gate: bfloat16 [2048], replicated, may hold values from -0.125 to 0.125
Outputs:
- layer_out: bfloat16 [128, 2048], P('ep')
- new_state: float32 [128, 16, 128, 128], P('ep', 'tp')
The draws below stay inside these ranges and needn't reach their ends.
Inputs may be any that keep to these rules, and one draw needn't show every extreme that they name: `routes`: each row names 4 different experts. Among the rows of one aligned block of 16 rows no expert is named more than 16 times, and some block reaches it: one expert is named exactly 16 times there.
All inputs are finite; a program needn't handle non-finite values.
Results may differ from the reference program's by a relative error of at most 0.019.
Values may be sent and summed in bfloat16 or wider, within the bound.
A program may use at most 64 MiB of HBM per device.

```python
import math
import jax
import jax.numpy as jnp
import numpy as np
from jax import lax

D = 2048
DK = 128
DV = 128
HK = 8
HV = 16
D_EXPERT = 512
D_SHARED = 512
TOPK = 4
SEQ_DEV = 16
SEQS = 128
EXPERTS = 8
CAP = 16
N_EP = 8
N_TP = 4


def levels(stream_key, dims, shards, smallest, high):
    def one(position, blocks):
        draws = jax.random.uniform(jax.random.fold_in(jax.random.fold_in(stream_key, 6), position), (blocks,), jnp.float32, smallest / len(shards), high / len(shards))
        return jnp.repeat(jnp.exp(draws), dims[position] // blocks).reshape((-1,) + (1,) * (len(dims) - position - 1))

    level = one(*shards[0])
    for cut in shards[1:]:
        level = level * one(*cut)
    return level


def routed_block(stream_key, own, number, rows, number_of, top, most, slope):
    sequence = jax.random.permutation(stream_key, number_of)
    heavy_load, ordinary = shares(number_of, rows * top, most, slope, True), shares(number_of, rows * top, most, slope, False)
    places = jnp.arange(number_of)

    def named(sizes, turn):
        used = int((sizes > 0).sum())
        fixed = max(1, used // 4)
        shifted = fixed + (places - fixed + turn * (used - fixed)) % max(1, number_of - fixed)
        return jnp.zeros((number_of,), jnp.int32).at[sequence[jnp.where(places < fixed, places, shifted)]].set(jnp.asarray(sizes, jnp.int32))

    sizes = jnp.where(number % 4 == 0, named(heavy_load, number // 4), named(ordinary, number - number // 4 - 1))
    mixed = jax.random.permutation(jax.random.fold_in(own, 3), number_of)
    source_of, taker = mixed[0:number_of // 2 * 2:2], mixed[1:number_of // 2 * 2:2]
    margin = jnp.minimum(sizes[source_of] - 1, most - sizes[taker]) // 2
    margin = jnp.where((source_of == sequence[0]) | (taker == sequence[0]) | (sizes[taker] == 0), 0, jnp.maximum(margin, 0))
    shifted = jax.random.randint(jax.random.fold_in(own, 4), (number_of // 2,), 0, 1 << 20) % (margin + 1)
    sizes = sizes.at[source_of].add(-shifted).at[taker].add(shifted)
    items = jnp.searchsorted(jnp.cumsum(sizes), jnp.arange(rows * top), side="right").astype(jnp.int32)
    table = items.reshape(top, rows).T
    table = table[jax.random.permutation(jax.random.fold_in(own, 1), rows)]
    turn = jax.random.randint(jax.random.fold_in(own, 2), (rows, 1), 0, top)
    return jnp.take_along_axis(table, (jnp.arange(top)[None, :] + turn) % top, axis=1)


def shares(count, total, most, lean, full):
    loads = [(1 << 20) // math.isqrt(standing ** lean) + 1 for standing in range(1, count + 1)]
    largest = most if full else min(most, max(-(-total // count), total * loads[0] // sum(loads)))
    least = 1 if total - largest >= count - 1 else 0
    given, rest = [largest] + [least] * (count - 1), total - largest - least * (count - 1)
    while rest > 0:
        free = [i for i in range(1, count) if given[i] < largest] or [i for i in range(1, count) if given[i] < most]
        pool, left = sum([loads[i] for i in free]), rest
        for i in free:
            extra = min(most - given[i], max(1, left * loads[i] // pool), rest)
            given[i] = given[i] + extra
            rest = rest - extra
    return np.array(given)


def noise(stream_key, extent, deviation, reach, pieces=(), held_as=jnp.bfloat16):
    values = jax.random.normal(stream_key, extent, jnp.float32) * deviation
    if len(pieces) > 0:
        values = levels(stream_key, extent, pieces, -0.22, 0.18) * values
    return jnp.clip(values, min=-reach, max=reach).astype(held_as)


def setup_inputs(seed: int = 0) -> dict:
    key_of = jax.random.split(jax.random.key(seed), 24)
    tokens = noise(key_of[0], (SEQS, D), 1.0, 6.0, ((0, 8),))
    norm_gain = jnp.clip(1.0 + 0.18 * jax.random.normal(key_of[1], (D,), jnp.float32), 0.099609375, 1.8984375).astype(jnp.bfloat16)
    query_weight = noise(key_of[2], (D, HK * DK), D ** -0.5, 0.125, ((0, 8), (1, 4)))
    key_weight = noise(key_of[3], (D, HK * DK), D ** -0.5, 0.125, ((0, 8), (1, 4)))
    value_weight = noise(key_of[4], (D, HV * DV), D ** -0.5, 0.125, ((0, 8), (1, 4)))
    outgate_weight = noise(key_of[5], (D, HV * DV), D ** -0.5, 0.125, ((0, 8), (1, 4)))
    beta_weight = noise(key_of[6], (D, HV), D ** -0.5, 0.125)
    decay_weight = noise(key_of[7], (D, HV), D ** -0.5, 0.125)
    decay_rate = jnp.clip(jnp.exp(math.log(6.0) - 5.7037825 * jax.random.uniform(key_of[8], (HV,), jnp.float32) ** levels(key_of[8], (HV,), ((0, 4),), -0.2, 0.2)), 0.02, 6.0)
    decay_bias = noise(key_of[9], (HV,), 1.0, 3.0, ((0, 4),), jnp.float32)
    head_gain = jnp.clip(1.0 + 0.18 * jax.random.normal(key_of[10], (DV,), jnp.float32), 0.099609375, 1.8984375).astype(jnp.bfloat16)
    recurrent = noise(key_of[11], (SEQS, HV, DK, DV), 0.5, 3.0, ((0, 8), (1, 4)), jnp.float32)
    output_weight = noise(key_of[12], (HV * DV, D), (HV * DV) ** -0.5, 0.125, ((0, 4), (1, 8)))
    ffn_gain = jnp.clip(1.0 + 0.18 * jax.random.normal(key_of[13], (D,), jnp.float32), 0.099609375, 1.8984375).astype(jnp.bfloat16)
    routes_keys = jax.random.split(jax.random.fold_in(key_of[14], 1), SEQS // SEQ_DEV)
    routes_turns = jax.random.permutation(jax.random.fold_in(key_of[14], 3), SEQS // SEQ_DEV)
    routes = jax.vmap(lambda own, number: routed_block(jax.random.fold_in(key_of[14], 2), own, number, SEQ_DEV, EXPERTS, TOPK, CAP, 2))(routes_keys, routes_turns).reshape((SEQS, TOPK))
    route_weight = jnp.clip(jnp.exp(math.log(1.0) - 2.3025851 * jax.random.uniform(key_of[15], (SEQS, TOPK), jnp.float32) ** levels(key_of[15], (SEQS, TOPK), ((0, 8),), -0.2, 0.2)), 0.1, 1.0)
    expert_gate = noise(key_of[16], (EXPERTS, D, D_EXPERT), D ** -0.5, 0.125, ((0, 8), (2, 4)))
    expert_up = noise(key_of[17], (EXPERTS, D, D_EXPERT), D ** -0.5, 0.125, ((0, 8), (2, 4)))
    expert_down = noise(key_of[18], (EXPERTS, D_EXPERT, D), D_EXPERT ** -0.5, 0.25, ((0, 8), (1, 4)))
    shared_gate = noise(key_of[19], (D, D_SHARED), D ** -0.5, 0.125, ((0, 8), (1, 4)))
    shared_up = noise(key_of[20], (D, D_SHARED), D ** -0.5, 0.125, ((0, 8), (1, 4)))
    shared_down = noise(key_of[21], (D_SHARED, D), D_SHARED ** -0.5, 0.25, ((0, 4), (1, 8)))
    branch_gate = noise(key_of[22], (D,), D ** -0.5, 0.125)
    return dict(tokens=tokens, norm_gain=norm_gain, query_weight=query_weight, key_weight=key_weight, value_weight=value_weight, outgate_weight=outgate_weight, beta_weight=beta_weight, decay_weight=decay_weight, decay_rate=decay_rate, decay_bias=decay_bias, head_gain=head_gain, recurrent=recurrent, output_weight=output_weight, ffn_gain=ffn_gain, routes=routes, route_weight=route_weight, expert_gate=expert_gate, expert_up=expert_up, expert_down=expert_down, shared_gate=shared_gate, shared_up=shared_up, shared_down=shared_down, branch_gate=branch_gate)


EPS = 1e-06
ROUTED_SCALE = 2.5

def rms_scale(values, gain):
    values = values.astype(jnp.float32)
    return values * lax.rsqrt(lax.optimization_barrier(jnp.mean(values * values, axis=-1, keepdims=True)) + EPS) * gain.astype(jnp.float32)

def unit_rows(values):
    return values * lax.rsqrt(lax.optimization_barrier(jnp.sum(values * values, axis=-1, keepdims=True)) + EPS)

def grouped_product(left, right, groups):
    inner = left.shape[1] // groups
    running = jnp.zeros((left.shape[0], right.shape[1]), jnp.float32)
    for index in range(groups):
        partial_product = jnp.dot(left[:, index * inner:(index + 1) * inner], right[index * inner:(index + 1) * inner], preferred_element_type=jnp.float32)
        running = running + partial_product.astype(jnp.bfloat16).astype(jnp.float32)
    return running

def reference(tokens, norm_gain, query_weight, key_weight, value_weight, outgate_weight, beta_weight, decay_weight, decay_rate, decay_bias, head_gain, recurrent, output_weight, ffn_gain, routes, route_weight, expert_gate, expert_up, expert_down, shared_gate, shared_up, shared_down, branch_gate):
    seqs, width = tokens.shape
    heads, key_dim, value_dim = (recurrent.shape[1], recurrent.shape[2], recurrent.shape[3])
    key_heads = query_weight.shape[1] // key_dim
    normed = rms_scale(tokens, norm_gain).astype(jnp.bfloat16)
    query_proj = jnp.dot(normed, query_weight, preferred_element_type=jnp.float32).astype(jnp.bfloat16)
    key_proj = jnp.dot(normed, key_weight, preferred_element_type=jnp.float32).astype(jnp.bfloat16)
    value_proj = jnp.dot(normed, value_weight, preferred_element_type=jnp.float32).astype(jnp.bfloat16)
    gate_proj = jnp.dot(normed, outgate_weight, preferred_element_type=jnp.float32).astype(jnp.bfloat16)
    beta_logit = jnp.dot(normed, beta_weight, preferred_element_type=jnp.float32)
    decay_logit = jnp.dot(normed, decay_weight, preferred_element_type=jnp.float32)
    repeat_count = heads // key_heads
    queries = unit_rows(jax.nn.silu(query_proj.astype(jnp.float32)).reshape(seqs, key_heads, key_dim))
    queries = jnp.repeat(queries, repeat_count, axis=1) * key_dim ** (-0.5)
    key_rows = unit_rows(jax.nn.silu(key_proj.astype(jnp.float32)).reshape(seqs, key_heads, key_dim))
    key_rows = jnp.repeat(key_rows, repeat_count, axis=1)
    value_rows = jax.nn.silu(value_proj.astype(jnp.float32)).reshape(seqs, heads, value_dim)
    strength = jax.nn.sigmoid(beta_logit)
    retain = jnp.exp(-decay_rate[None, :] * jax.nn.softplus(decay_logit + decay_bias[None, :]))
    decayed = recurrent * retain[:, :, None, None]
    predicted = jnp.einsum('shde,shd->she', decayed, key_rows, precision=lax.Precision.HIGHEST)
    correction = strength[:, :, None] * (value_rows - predicted)
    new_state = decayed + key_rows[:, :, :, None] * correction[:, :, None, :]
    readout = jnp.einsum('shde,shd->she', new_state, queries, precision=lax.Precision.HIGHEST)
    out_gate = jax.nn.silu(gate_proj.astype(jnp.float32)).reshape(seqs, heads, value_dim)
    heads_out = (rms_scale(readout, head_gain) * out_gate).astype(jnp.bfloat16).reshape(seqs, heads * value_dim)
    mix = grouped_product(heads_out, output_weight, N_TP)
    residual = (tokens.astype(jnp.float32) + mix).astype(jnp.bfloat16)
    ffn_in = rms_scale(residual, ffn_gain).astype(jnp.bfloat16)
    topk = routes.shape[1]
    seq_local = seqs // N_EP
    experts_total = expert_gate.shape[0]
    pair_count = seq_local * topk
    pair_ids = routes.reshape(N_EP, pair_count).astype(jnp.int32)
    onehot = (pair_ids[:, :, None] == jnp.arange(experts_total).astype(jnp.int32)[None, None, :]).astype(jnp.int32)
    slots = lax.optimization_barrier(jnp.sum((jnp.cumsum(onehot, axis=1) - onehot) * onehot, axis=2)).astype(jnp.int32)
    target = (pair_ids * CAP + slots).astype(jnp.int32)
    source_rows = jnp.repeat(ffn_in.reshape(N_EP, seq_local, width), topk, axis=1)
    buffer = jnp.zeros((N_EP, experts_total * CAP, width), jnp.bfloat16)
    source_index = jnp.arange(N_EP).astype(jnp.int32)[:, None]
    buffer = buffer.at[source_index, target].set(source_rows)
    buffer = buffer.reshape(N_EP, experts_total, CAP, width).transpose(1, 0, 2, 3).reshape(experts_total, N_EP * CAP, width)

    def expert_rows(operands):
        rows_in, gate_matrix, up_matrix, down_matrix = operands
        gate_part = jnp.dot(rows_in, gate_matrix, preferred_element_type=jnp.float32)
        up_part = jnp.dot(rows_in, up_matrix, preferred_element_type=jnp.float32)
        act = (jax.nn.silu(gate_part) * up_part).astype(jnp.bfloat16)
        return grouped_product(act, down_matrix, N_TP).astype(jnp.bfloat16)
    results = lax.map(expert_rows, (buffer, expert_gate, expert_up, expert_down))
    results = results.reshape(experts_total, N_EP, CAP, width).transpose(1, 0, 2, 3).reshape(N_EP, experts_total * CAP, width)
    pair_out = jnp.take_along_axis(results, target[:, :, None], axis=1).astype(jnp.float32)
    scaled = route_weight / lax.optimization_barrier(jnp.sum(route_weight, axis=1, keepdims=True)) * ROUTED_SCALE
    moe = lax.optimization_barrier(jnp.sum(pair_out.reshape(seqs, topk, width) * scaled[:, :, None], axis=1))
    shared_g = jnp.dot(ffn_in, shared_gate, preferred_element_type=jnp.float32)
    shared_u = jnp.dot(ffn_in, shared_up, preferred_element_type=jnp.float32)
    shared_act = (jax.nn.silu(shared_g) * shared_u).astype(jnp.bfloat16)
    shared_out = grouped_product(shared_act, shared_down, N_TP)
    branch = jax.nn.sigmoid(jnp.dot(ffn_in, branch_gate, preferred_element_type=jnp.float32))
    layer_out = (residual.astype(jnp.float32) + moe + branch[:, None] * shared_out).astype(jnp.bfloat16)
    return (layer_out, new_state)
```

```python
import functools

import jax
import jax.numpy as jnp
from jax import lax
from jax.experimental import pallas as pl
from jax.experimental.pallas import tpu as pltpu
from jax.sharding import PartitionSpec as P

EPS = 1e-06
ROUTED_SCALE = 2.5
MESH = pl.DeviceIdType.MESH
F32 = jnp.float32
BF16 = jnp.bfloat16
STEP = 4


def silu(v):
    return v / (1.0 + jnp.exp(-v))


def sigmoid(v):
    return 1.0 / (1.0 + jnp.exp(-v))


def rms_scale(values, gain):
    values = values.astype(F32)
    return (
        values
        * lax.rsqrt(jnp.mean(values * values, axis=-1, keepdims=True) + EPS)
        * gain.astype(F32)
    )


def unit_rows(values):
    return values * lax.rsqrt(jnp.sum(values * values, axis=-1, keepdims=True) + EPS)


def dot_nt(a, b):
    return lax.dot_general(a, b, (((1,), (1,)), ((), ())), preferred_element_type=F32)


def remote(src, dst, send_sem, recv_sem, e, t):
    return pltpu.make_async_remote_copy(
        src_ref=src,
        dst_ref=dst,
        send_sem=send_sem,
        recv_sem=recv_sem,
        device_id=(e, t),
        device_id_type=MESH,
    )


def loop(lo, hi, body):
    def step(i, c):
        body(i)
        return c

    lax.fori_loop(lo, hi, step, 0)


def project_kernel(
    n,
    key_dim,
    tokens_ref,
    gain_ref,
    qw_ref,
    kw_ref,
    vw_ref,
    gw_ref,
    wbd_ref,
    rate_ref,
    bias_ref,
    routes_ref,
    rw_ref,
    kq_ref,
    value_ref,
    gate_ref,
    scalars_ref,
    route_ref,
    weights,
    xsend,
    xbuf,
    pbuf,
    rbuf,
    wsem,
    xs,
    xr,
    ps,
    pr,
):
    me, tp = lax.axis_index("ep"), lax.axis_index("tp")
    rows = tokens_ref.shape[0]
    qc, vc = qw_ref.shape[1], vw_ref.shape[1]
    total = 2 * qc + 2 * vc
    depth = qw_ref.shape[0]
    fetches = []
    at = 0
    for i, w in enumerate((qw_ref, kw_ref, vw_ref, gw_ref)):
        c = pltpu.make_async_copy(w, weights.at[:, pl.ds(at, w.shape[1])], wsem.at[i])
        c.start()
        fetches.append(c)
        at += w.shape[1]

    barrier = pltpu.get_barrier_semaphore()

    def greet(i):
        pl.semaphore_signal(
            barrier, inc=1, device_id=(lax.rem(me + i, n), tp), device_id_type=MESH
        )

    loop(1, n, greet)

    normed = rms_scale(tokens_ref[...], gain_ref[...]).astype(BF16)
    for e in range(n):
        xsend[e] = normed[:, e * depth : (e + 1) * depth]
    pl.semaphore_wait(barrier, n - 1)

    def send_x(i):
        p = lax.rem(me + i, n)
        remote(xsend.at[p], xbuf.at[me], xs.at[i], xr.at[me], p, tp).start()

    loop(1, n, send_x)
    xbuf[me] = xsend[me]

    logits = dot_nt(normed, wbd_ref[...])
    heads = logits.shape[1] // 2
    strength = sigmoid(logits[:, :heads])
    shifted = logits[:, heads:] + bias_ref[...]
    softplus = jnp.maximum(shifted, 0.0) + jnp.log1p(jnp.exp(-jnp.abs(shifted)))
    retain = jnp.exp(-rate_ref[...] * softplus)
    rw = rw_ref[...]
    scaled = rw / jnp.sum(rw, axis=1, keepdims=True) * ROUTED_SCALE
    routes = routes_ref[...]
    lane = lax.broadcasted_iota(jnp.int32, (rows, 128), 1)
    for e in range(n):
        w = jnp.sum(jnp.where(routes == e, scaled, 0.0), axis=1, keepdims=True)
        high = w.astype(BF16).astype(F32)
        pbuf[e, :, total:] = jnp.where(lane < 64, high, w - high).astype(BF16)

    for c in fetches:
        c.wait()

    def got_x(i):
        p = lax.rem(me + i, n)
        remote(xbuf.at[p], xbuf.at[p], xs.at[i], xr.at[p], p, tp).wait_recv()

    loop(1, n, got_x)
    x = xbuf[...].reshape(n * rows, depth)
    part = 512
    for c in range(0, total, part):
        width = min(part, total - c)
        out = jnp.dot(x, weights[:, c : c + width], preferred_element_type=F32)
        pbuf[:, :, c : c + width] = out.astype(BF16).reshape(n, rows, width)

    def send_p(i):
        p = lax.rem(me + i, n)
        remote(pbuf.at[p], rbuf.at[me], ps.at[i], pr.at[me], p, tp).start()

    loop(1, n, send_p)
    rbuf[me] = pbuf[me]

    def got_p(i):
        p = lax.rem(me + i, n)
        remote(rbuf.at[p], rbuf.at[p], ps.at[i], pr.at[p], p, tp).wait_recv()

    loop(1, n, got_p)

    def gathered(c, width):
        acc = rbuf[0, :, c : c + width].astype(F32)
        for e in range(1, n):
            acc = acc + rbuf[e, :, c : c + width].astype(F32)
        return acc.astype(BF16).astype(F32)

    keys = qc // key_dim
    q_rows = [
        unit_rows(silu(gathered(j * key_dim, key_dim))) * key_dim ** (-0.5)
        for j in range(keys)
    ]
    k_rows = [unit_rows(silu(gathered(qc + j * key_dim, key_dim))) for j in range(keys)]
    for j in range(0, vc, 128):
        value_ref[:, j : j + 128] = silu(gathered(2 * qc + j, 128))
        gate_ref[:, j : j + 128] = silu(gathered(2 * qc + vc + j, 128))
    stacked = q_rows + k_rows
    stacked.append(jnp.zeros((128 - 2 * keys * rows, key_dim), F32))
    kq_ref[...] = jnp.concatenate(stacked, axis=0).T
    lane = lax.broadcasted_iota(jnp.int32, scalars_ref.shape, 1)
    scalars = jnp.zeros(scalars_ref.shape, F32)
    for h in range(heads):
        scalars = jnp.where(lane == h, retain[:, h : h + 1], scalars)
        scalars = jnp.where(lane == heads + h, strength[:, h : h + 1], scalars)
    for j in range(keys):
        qk = jnp.sum(q_rows[j] * k_rows[j], axis=1, keepdims=True)
        scalars = jnp.where(lane == 2 * heads + j, qk, scalars)
    scalars_ref[...] = scalars
    for e in range(n):
        w = rbuf[e, :, total:].astype(F32)
        route_ref[e * rows : (e + 1) * rows, :] = jnp.broadcast_to(
            w[:, 0:1] + w[:, 64:65], (rows, 128)
        )

    def sent(i):
        p = lax.rem(me + i, n)
        remote(xsend.at[p], xbuf.at[me], xs.at[i], xr.at[me], p, tp).wait_send()
        remote(pbuf.at[p], rbuf.at[me], ps.at[i], pr.at[me], p, tp).wait_send()

    loop(1, n, sent)


def delta_kernel(
    keys, rows, scalars_ref, kq_ref, value_ref, state_ref, new_ref, read_ref, held
):
    g = pl.program_id(0)
    heads = state_ref.shape[1]
    key_dim, value_dim = state_ref.shape[2], state_ref.shape[3]
    turned = pltpu.roll(kq_ref[...], lax.rem(128 - STEP * g, 128), 1)
    values = pltpu.roll(value_ref[...], lax.rem(rows - STEP * g, rows), 0)
    for i in range(STEP):
        s = STEP * g + i
        for j in range(keys):
            q = jnp.broadcast_to(
                turned[:, j * rows + i : j * rows + i + 1], (key_dim, value_dim)
            )
            at = (keys + j) * rows + i
            k = jnp.broadcast_to(turned[:, at : at + 1], (key_dim, value_dim))
            qk = scalars_ref[s, 2 * heads + j]
            for h in range(j * (heads // keys), (j + 1) * (heads // keys)):
                cols = slice(h * value_dim, (h + 1) * value_dim)
                retain, strength = scalars_ref[s, h], scalars_ref[s, heads + h]
                decayed = state_ref[i, h] * retain
                predicted = jnp.sum(decayed * k, axis=0, keepdims=True)
                before = jnp.sum(decayed * q, axis=0, keepdims=True)
                correction = strength * (values[i : i + 1, cols] - predicted)
                new_ref[i, h] = decayed + k * correction
                held[i : i + 1, cols] = before + qk * correction
    row = lax.broadcasted_iota(jnp.int32, held.shape, 0)
    mine = (row >= STEP * g) & (row < STEP * (g + 1))
    read_ref[...] = jnp.where(mine, pltpu.roll(held[...], STEP * g, 0), read_ref[...])


def mix_kernel(
    n,
    m,
    read_ref,
    gate_ref,
    head_gain_ref,
    tokens_ref,
    ow_ref,
    ffn_gain_ref,
    eg_ref,
    eu_ref,
    ed_ref,
    shared_ref,
    branch_ref,
    route_ref,
    out_ref,
    ow,
    eg,
    eu,
    ed,
    hbuf,
    mbuf,
    mrecv,
    sbuf,
    resid,
    fbuf,
    pbuf,
    srecv,
    rsend,
    rrecv,
    obuf,
    wsem,
    hs,
    hr,
    ms,
    mr,
    ss,
    sr,
    fs,
    fr,
    gs,
    gr,
    bs,
    br,
    rs,
    rr,
    os_,
    or_,
):
    me, tp = lax.axis_index("ep"), lax.axis_index("tp")
    count = n * m
    lin = me * m + tp
    half = m // 2
    core = lax.rem(tp, 2)
    pair = tp + 1 - 2 * core
    rows, width = tokens_ref.shape
    fetches = []
    for i, (w, v) in enumerate(((ow_ref, ow), (eg_ref, eg), (eu_ref, eu), (ed_ref, ed))):
        c = pltpu.make_async_copy(w, v, wsem.at[i])
        c.start()
        fetches.append(c)

    barrier = pltpu.get_barrier_semaphore()

    def greet(i):
        p = lax.rem(lin + i, count)
        pl.semaphore_signal(
            barrier, inc=1, device_id=(p // m, lax.rem(p, m)), device_id_type=MESH
        )

    loop(1, count, greet)

    value_dim = head_gain_ref.shape[1]
    for h in range(0, read_ref.shape[1], value_dim):
        cols = slice(h, h + value_dim)
        hbuf[me, :, cols] = (
            rms_scale(read_ref[:, cols], head_gain_ref[...]) * gate_ref[:, cols]
        ).astype(BF16)
    pl.semaphore_wait(barrier, count - 1)

    def send_h(i):
        p = lax.rem(me + i, n)
        remote(hbuf.at[me], hbuf.at[me], hs.at[i], hr.at[me], p, tp).start()

    loop(1, n, send_h)
    fetches[0].wait()

    def got_h(i):
        p = lax.rem(me + i, n)
        remote(hbuf.at[p], hbuf.at[p], hs.at[i], hr.at[p], p, tp).wait_recv()

    loop(1, n, got_h)
    h_all = hbuf[...].reshape(n * rows, hbuf.shape[2])
    block = ow.shape[1]
    mbuf[...] = (
        jnp.dot(h_all, ow[...], preferred_element_type=F32).astype(BF16).reshape(n, rows, block)
    )

    def send_m(i):
        p = lax.rem(lin + i, count)
        e, t = p // m, lax.rem(p, m)
        remote(mbuf.at[e], mrecv.at[lin], ms.at[i], mr.at[lin], e, t).start()

    loop(1, count, send_m)
    mrecv[lin] = mbuf[me]

    def send_s(i):
        p = lax.rem(me + i, n)
        remote(shared_ref.at[p], sbuf.at[me], ss.at[i], sr.at[me], p, tp).start()

    loop(1, n, send_s)
    sbuf[me] = shared_ref[me]

    def got_m(i):
        p = lax.rem(lin + i, count)
        e, t = p // m, lax.rem(p, m)
        remote(mrecv.at[p], mrecv.at[p], ms.at[i], mr.at[p], e, t).wait_recv()

    loop(1, count, got_m)
    pieces = []
    for e in range(n):
        acc = mrecv[e * m].astype(F32)
        for t in range(1, m):
            acc = acc + mrecv[e * m + t].astype(F32)
        pieces.append(acc)
    mix = jnp.concatenate(pieces, axis=1)
    residual = (tokens_ref[...].astype(F32) + mix).astype(BF16).astype(F32)
    quarter = width // m
    for t in range(m):
        resid[t] = residual[:, t * quarter : (t + 1) * quarter]
    ffn_in = rms_scale(residual, ffn_gain_ref[...]).astype(BF16)
    split = width // 2
    fbuf[0, me] = ffn_in[:, :split]
    fbuf[1, me] = ffn_in[:, split:]

    def send_f(i):
        p = lax.rem(me + i, n)
        remote(
            fbuf.at[core, me], fbuf.at[core, me], fs.at[i], fr.at[core, me], p, tp
        ).start()

    loop(1, n, send_f)

    def pass_f(i):
        p = lax.rem(me + n - i, n)
        mine = fbuf.at[core, p]
        remote(mine, mine, fs.at[i], fr.at[core, p], p, tp).wait_recv()
        remote(mine, mine, gs.at[i], gr.at[p], me, pair).start()

    loop(1, n, pass_f)

    def got_s(i):
        p = lax.rem(me + i, n)
        remote(sbuf.at[p], sbuf.at[p], ss.at[i], sr.at[p], p, tp).wait_recv()

    loop(1, n, got_s)
    units = sbuf.shape[1] // 3
    shared = jnp.concatenate([sbuf[e] for e in range(n)], axis=1)
    for c in fetches[1:]:
        c.wait()

    def got_f(i):
        p = lax.rem(me + n - i, n)
        other = fbuf.at[1 - core, p]
        remote(other, other, gs.at[i], gr.at[p], me, pair).wait_recv()

    loop(1, n, got_f)

    x0 = fbuf[0].reshape(n * rows, split)
    x1 = fbuf[1].reshape(n * rows, split)

    def up(w):
        return jnp.dot(x0, w[0, :split], preferred_element_type=F32) + jnp.dot(
            x1, w[0, split:], preferred_element_type=F32
        )

    def up_shared(w):
        return dot_nt(x0, w[:, :split]) + dot_nt(x1, w[:, split:])

    act = (silu(up(eg)) * up(eu)).astype(BF16)
    shared_act = (
        silu(up_shared(shared[:units])) * up_shared(shared[units : 2 * units])
    ).astype(BF16)
    bg = branch_ref[...].astype(F32)
    branch = sigmoid(
        jnp.sum(x0.astype(F32) * bg[:, :split], axis=1, keepdims=True)
        + jnp.sum(x1.astype(F32) * bg[:, split:], axis=1, keepdims=True)
    )
    weight = route_ref[:, 0:1]
    for c in range(2):
        cols = slice(c * split, (c + 1) * split)
        out = weight * jnp.dot(act, ed[0, :, cols], preferred_element_type=F32)
        out = out + branch * jnp.dot(
            shared_act, shared[2 * units :, cols], preferred_element_type=F32
        )
        pbuf[c] = out.astype(BF16)

    swap = remote(pbuf.at[1 - core], srecv, bs.at[0], br.at[0], me, pair)
    swap.start()
    swap.wait_recv()
    for e in range(n):
        these = slice(e * rows, (e + 1) * rows)
        both = pbuf[core, these].astype(F32) + srecv[these].astype(F32)
        for x in range(half):
            rsend[e * half + x] = both[:, x * quarter : (x + 1) * quarter].astype(BF16)

    blocks = n * half
    mine = me * half + tp // 2

    def send_r(i):
        p = lax.rem(mine + i, blocks)
        e, x = p // half, lax.rem(p, half)
        remote(rsend.at[p], rrecv.at[mine], rs.at[i], rr.at[mine], e, 2 * x + core).start()

    loop(1, blocks, send_r)
    rrecv[mine] = rsend[mine]

    def got_r(i):
        p = lax.rem(mine + i, blocks)
        e, x = p // half, lax.rem(p, half)
        remote(rrecv.at[p], rrecv.at[p], rs.at[i], rr.at[p], e, 2 * x + core).wait_recv()

    loop(1, blocks, got_r)
    place = core * half + tp // 2
    acc = resid[place]
    for p in range(blocks):
        acc = acc + rrecv[p].astype(F32)
    obuf[place] = acc.astype(BF16)

    def send_o(i):
        t = lax.rem(tp + i, m)
        remote(obuf.at[place], obuf.at[place], os_.at[i], or_.at[place], me, t).start()

    loop(1, m, send_o)

    def got_o(i):
        t = lax.rem(tp + i, m)
        there = lax.rem(t, 2) * half + t // 2
        remote(obuf.at[there], obuf.at[there], os_.at[i], or_.at[there], me, t).wait_recv()

    loop(1, m, got_o)
    for t in range(m):
        out_ref[:, t * quarter : (t + 1) * quarter] = obuf[t]

    def sent_ep(i):
        p = lax.rem(me + i, n)
        remote(hbuf.at[me], hbuf.at[me], hs.at[i], hr.at[me], p, tp).wait_send()
        remote(shared_ref.at[p], sbuf.at[me], ss.at[i], sr.at[me], p, tp).wait_send()
        remote(
            fbuf.at[core, me], fbuf.at[core, me], fs.at[i], fr.at[core, me], p, tp
        ).wait_send()
        b = lax.rem(me + n - i, n)
        remote(fbuf.at[core, b], fbuf.at[core, b], gs.at[i], gr.at[b], me, pair).wait_send()

    loop(1, n, sent_ep)

    def sent_m(i):
        p = lax.rem(lin + i, count)
        e, t = p // m, lax.rem(p, m)
        remote(mbuf.at[e], mrecv.at[lin], ms.at[i], mr.at[lin], e, t).wait_send()

    loop(1, count, sent_m)
    swap.wait_send()

    def sent_r(i):
        p = lax.rem(mine + i, blocks)
        e, x = p // half, lax.rem(p, half)
        remote(
            rsend.at[p], rrecv.at[mine], rs.at[i], rr.at[mine], e, 2 * x + core
        ).wait_send()

    loop(1, blocks, sent_r)

    def sent_o(i):
        t = lax.rem(tp + i, m)
        remote(obuf.at[place], obuf.at[place], os_.at[i], or_.at[place], me, t).wait_send()

    loop(1, m, sent_o)


VMEM = pl.BlockSpec(memory_space=pltpu.VMEM)
ANY = pl.BlockSpec(memory_space=pl.ANY)


def per_device(
    n,
    m,
    tokens,
    norm_gain,
    query_weight,
    key_weight,
    value_weight,
    outgate_weight,
    beta_weight,
    decay_weight,
    decay_rate,
    decay_bias,
    head_gain,
    recurrent,
    output_weight,
    ffn_gain,
    routes,
    route_weight,
    expert_gate,
    expert_up,
    expert_down,
    shared_gate,
    shared_up,
    shared_down,
    branch_gate,
):
    rows, width = tokens.shape
    _, heads, key_dim, value_dim = recurrent.shape
    depth, qc = query_weight.shape
    vc = value_weight.shape[1]
    keys = qc // key_dim
    total = 2 * qc + 2 * vc
    sds = jax.ShapeDtypeStruct
    dma = pltpu.SemaphoreType.DMA
    start = lax.axis_index("tp") * heads
    wbd = jnp.concatenate(
        (
            lax.dynamic_slice_in_dim(beta_weight, start, heads, 1),
            lax.dynamic_slice_in_dim(decay_weight, start, heads, 1),
        ),
        axis=1,
    ).T
    units = shared_gate.shape[1] // n
    cols = shared_down.shape[1]
    shared = jnp.concatenate(
        (
            shared_gate.T.reshape(n, units, depth),
            shared_up.T.reshape(n, units, depth),
            shared_down.reshape(n, units, cols),
        ),
        axis=1,
    )
    kq, value, gate, scalars, route = pl.pallas_call(
        functools.partial(project_kernel, n, key_dim),
        out_shape=(
            sds((key_dim, 128), F32),
            sds((rows, vc), F32),
            sds((rows, vc), F32),
            sds((rows, 2 * heads + keys), F32),
            sds((n * rows, 128), F32),
        ),
        in_specs=[VMEM] * 2 + [ANY] * 4 + [VMEM] * 5,
        out_specs=(VMEM,) * 5,
        scratch_shapes=[
            pltpu.VMEM((depth, total), BF16),
            pltpu.VMEM((n, rows, depth), BF16),
            pltpu.VMEM((n, rows, depth), BF16),
            pltpu.VMEM((n, rows, total + 128), BF16),
            pltpu.VMEM((n, rows, total + 128), BF16),
            dma((4,)),
            dma((n,)),
            dma((n,)),
            dma((n,)),
            dma((n,)),
        ],
        compiler_params=pltpu.CompilerParams(collective_id=0, has_side_effects=True),
    )(
        tokens,
        norm_gain[None, :],
        query_weight,
        key_weight,
        value_weight,
        outgate_weight,
        wbd,
        decay_rate[None, :],
        decay_bias[None, :],
        routes,
        route_weight,
    )

    new_state, readout = pl.pallas_call(
        functools.partial(delta_kernel, keys, rows),
        out_shape=(sds(recurrent.shape, F32), sds((rows, vc), F32)),
        grid=(rows // STEP,),
        in_specs=[
            pl.BlockSpec(memory_space=pltpu.SMEM),
            pl.BlockSpec((key_dim, 128), lambda g: (0, 0)),
            pl.BlockSpec((rows, vc), lambda g: (0, 0)),
            pl.BlockSpec((STEP, heads, key_dim, value_dim), lambda g: (g, 0, 0, 0)),
        ],
        out_specs=(
            pl.BlockSpec((STEP, heads, key_dim, value_dim), lambda g: (g, 0, 0, 0)),
            pl.BlockSpec((rows, vc), lambda g: (0, 0)),
        ),
        scratch_shapes=[pltpu.VMEM((rows, vc), F32)],
        compiler_params=pltpu.CompilerParams(dimension_semantics=("arbitrary",)),
    )(scalars, kq, value, recurrent)

    quarter = width // m
    blocks = n * (m // 2)
    layer_out = pl.pallas_call(
        functools.partial(mix_kernel, n, m),
        out_shape=sds((rows, width), BF16),
        in_specs=[VMEM] * 4 + [ANY, VMEM] + [ANY] * 3 + [VMEM] * 3,
        out_specs=VMEM,
        scratch_shapes=[
            pltpu.VMEM(output_weight.shape, BF16),
            pltpu.VMEM(expert_gate.shape, BF16),
            pltpu.VMEM(expert_up.shape, BF16),
            pltpu.VMEM(expert_down.shape, BF16),
            pltpu.VMEM((n, rows, vc), BF16),
            pltpu.VMEM((n, rows, cols), BF16),
            pltpu.VMEM((n * m, rows, cols), BF16),
            pltpu.VMEM(shared.shape, BF16),
            pltpu.VMEM((m, rows, quarter), F32),
            pltpu.VMEM((2, n, rows, width // 2), BF16),
            pltpu.VMEM((2, n * rows, width // 2), BF16),
            pltpu.VMEM((n * rows, width // 2), BF16),
            pltpu.VMEM((blocks, rows, quarter), BF16),
            pltpu.VMEM((blocks, rows, quarter), BF16),
            pltpu.VMEM((m, rows, quarter), BF16),
            dma((4,)),
            dma((n,)),
            dma((n,)),
            dma((n * m,)),
            dma((n * m,)),
            dma((n,)),
            dma((n,)),
            dma((n,)),
            dma((2, n)),
            dma((n,)),
            dma((n,)),
            dma((1,)),
            dma((1,)),
            dma((blocks,)),
            dma((blocks,)),
            dma((m,)),
            dma((m,)),
        ],
        compiler_params=pltpu.CompilerParams(collective_id=1, has_side_effects=True),
    )(
        readout,
        gate,
        head_gain[None, :],
        tokens,
        output_weight,
        ffn_gain[None, :],
        expert_gate,
        expert_up,
        expert_down,
        shared,
        branch_gate[None, :],
        route,
    )
    return (layer_out, new_state)


def solution(mesh):
    return jax.shard_map(
        functools.partial(per_device, mesh.shape["ep"], mesh.shape["tp"]),
        mesh=mesh,
        in_specs=(
            P("ep", None),
            P(),
            P("ep", "tp"),
            P("ep", "tp"),
            P("ep", "tp"),
            P("ep", "tp"),
            P(),
            P(),
            P("tp"),
            P("tp"),
            P(),
            P("ep", "tp", None, None),
            P("tp", "ep"),
            P(),
            P("ep", None),
            P("ep", None),
            P("ep", None, "tp"),
            P("ep", None, "tp"),
            P("ep", "tp", None),
            P("ep", "tp"),
            P("ep", "tp"),
            P("tp", "ep"),
            P(),
        ),
        out_specs=(P("ep", None), P("ep", "tp", None, None)),
        check_vma=False,
    )
```

```python
import functools

import jax
import jax.numpy as jnp
from jax import lax
from jax.experimental import pallas as pl
from jax.experimental.pallas import tpu as pltpu
from jax.sharding import PartitionSpec as P

EPS = 1e-06
ROUTED_SCALE = 2.5
MESH = pl.DeviceIdType.MESH
F32 = jnp.float32
BF16 = jnp.bfloat16
STEP = 4


def silu(v):
    return v / (1.0 + jnp.exp(-v))


def sigmoid(v):
    return 1.0 / (1.0 + jnp.exp(-v))


def rms_scale(values, gain):
    values = values.astype(F32)
    return (
        values
        * lax.rsqrt(jnp.mean(values * values, axis=-1, keepdims=True) + EPS)
        * gain.astype(F32).reshape(1, -1)
    )


def unit_rows(values):
    return values * lax.rsqrt(jnp.sum(values * values, axis=-1, keepdims=True) + EPS)


def dot_nt(a, b):
    return lax.dot_general(a, b, (((1,), (1,)), ((), ())), preferred_element_type=F32)


def remote(src, dst, send_sem, recv_sem, e, t):
    return pltpu.make_async_remote_copy(
        src_ref=src,
        dst_ref=dst,
        send_sem=send_sem,
        recv_sem=recv_sem,
        device_id=(e, t),
        device_id_type=MESH,
    )


def loop(lo, hi, body):
    def step(i, c):
        body(i)
        return c

    lax.fori_loop(lo, hi, step, 0)


def project_kernel(
    n,
    key_dim,
    tokens_ref,
    gain_ref,
    qw_ref,
    kw_ref,
    vw_ref,
    gw_ref,
    beta_ref,
    decay_ref,
    rate_ref,
    bias_ref,
    routes_ref,
    rw_ref,
    kq_ref,
    value_ref,
    gate_ref,
    scalars_ref,
    route_ref,
    weights,
    xsend,
    xbuf,
    pbuf,
    rbuf,
    wsem,
    xs,
    xr,
    ps,
    pr,
):
    me, tp = lax.axis_index("ep"), lax.axis_index("tp")
    rows = tokens_ref.shape[0]
    qc, vc = qw_ref.shape[1], vw_ref.shape[1]
    total = 2 * qc + 2 * vc
    depth = qw_ref.shape[0]
    fetches = []
    at = 0
    for i, w in enumerate((qw_ref, kw_ref, vw_ref, gw_ref)):
        c = pltpu.make_async_copy(w, weights.at[:, pl.ds(at, w.shape[1])], wsem.at[i])
        c.start()
        fetches.append(c)
        at += w.shape[1]

    barrier = pltpu.get_barrier_semaphore()

    def greet(i):
        pl.semaphore_signal(
            barrier, inc=1, device_id=(lax.rem(me + i, n), tp), device_id_type=MESH
        )

    loop(1, n, greet)

    normed = rms_scale(tokens_ref[...], gain_ref[...]).astype(BF16)
    for e in range(n):
        xsend[e] = normed[:, e * depth : (e + 1) * depth]
    pl.semaphore_wait(barrier, n - 1)

    def send_x(i):
        p = lax.rem(me + i, n)
        remote(xsend.at[p], xbuf.at[me], xs.at[i], xr.at[me], p, tp).start()

    loop(1, n, send_x)
    xbuf[me] = xsend[me]

    heads = rate_ref.shape[1]
    column = lax.broadcasted_iota(jnp.int32, (rows, beta_ref.shape[0]), 1)
    lane = lax.broadcasted_iota(jnp.int32, (rows, heads), 1)

    def own_heads(w):
        logits = dot_nt(normed, w)
        own = jnp.zeros((rows, heads), F32)
        for h in range(heads):
            kept = jnp.where(column == tp * heads + h, logits, 0.0)
            own = jnp.where(lane == h, jnp.sum(kept, axis=1, keepdims=True), own)
        return own

    strength = sigmoid(own_heads(beta_ref[...]))
    shifted = own_heads(decay_ref[...]) + bias_ref[...]
    softplus = jnp.maximum(shifted, 0.0) + jnp.log1p(jnp.exp(-jnp.abs(shifted)))
    retain = jnp.exp(-rate_ref[...] * softplus)
    rw = rw_ref[...]
    scaled = rw / jnp.sum(rw, axis=0, keepdims=True) * ROUTED_SCALE
    routes = routes_ref[...]
    expert = lax.broadcasted_iota(jnp.int32, (128, rows), 0)
    by_expert = jnp.zeros((128, rows), F32)
    for k in range(routes.shape[0]):
        by_expert = by_expert + jnp.where(
            expert == routes[k : k + 1, :], scaled[k : k + 1, :], 0.0
        )
    by_expert = by_expert.T
    lane = lax.broadcasted_iota(jnp.int32, (rows, 128), 1)
    for e in range(n):
        w = by_expert[:, e : e + 1]
        high = w.astype(BF16).astype(F32)
        pbuf[e, :, total:] = jnp.where(lane < 64, high, w - high).astype(BF16)

    for c in fetches:
        c.wait()

    def got_x(i):
        p = lax.rem(me + i, n)
        remote(xbuf.at[p], xbuf.at[p], xs.at[i], xr.at[p], p, tp).wait_recv()

    loop(1, n, got_x)
    x = xbuf[...].reshape(n * rows, depth)
    part = 512
    for c in range(0, total, part):
        width = min(part, total - c)
        out = jnp.dot(x, weights[:, c : c + width], preferred_element_type=F32)
        pbuf[:, :, c : c + width] = out.astype(BF16).reshape(n, rows, width)

    def send_p(i):
        p = lax.rem(me + i, n)
        remote(pbuf.at[p], rbuf.at[me], ps.at[i], pr.at[me], p, tp).start()

    loop(1, n, send_p)
    rbuf[me] = pbuf[me]

    def got_p(i):
        p = lax.rem(me + i, n)
        remote(rbuf.at[p], rbuf.at[p], ps.at[i], pr.at[p], p, tp).wait_recv()

    loop(1, n, got_p)

    def gathered(c, width):
        acc = rbuf[0, :, c : c + width].astype(F32)
        for e in range(1, n):
            acc = acc + rbuf[e, :, c : c + width].astype(F32)
        return acc.astype(BF16).astype(F32)

    keys = qc // key_dim
    q_rows = [
        unit_rows(silu(gathered(j * key_dim, key_dim))) * key_dim ** (-0.5)
        for j in range(keys)
    ]
    k_rows = [unit_rows(silu(gathered(qc + j * key_dim, key_dim))) for j in range(keys)]
    for j in range(0, vc, 128):
        value_ref[:, j : j + 128] = silu(gathered(2 * qc + j, 128))
        gate_ref[:, j : j + 128] = silu(gathered(2 * qc + vc + j, 128))
    stacked = q_rows + k_rows
    stacked.append(jnp.zeros((128 - 2 * keys * rows, key_dim), F32))
    kq_ref[...] = jnp.concatenate(stacked, axis=0).T
    lane = lax.broadcasted_iota(jnp.int32, scalars_ref.shape, 1)
    scalars = jnp.zeros(scalars_ref.shape, F32)
    for h in range(heads):
        scalars = jnp.where(lane == h, retain[:, h : h + 1], scalars)
        scalars = jnp.where(lane == heads + h, strength[:, h : h + 1], scalars)
    for j in range(keys):
        qk = jnp.sum(q_rows[j] * k_rows[j], axis=1, keepdims=True)
        scalars = jnp.where(lane == 2 * heads + j, qk, scalars)
    scalars_ref[...] = scalars
    for e in range(n):
        w = rbuf[e, :, total:].astype(F32)
        route_ref[e * rows : (e + 1) * rows, :] = jnp.broadcast_to(
            w[:, 0:1] + w[:, 64:65], (rows, 128)
        )

    def sent(i):
        p = lax.rem(me + i, n)
        remote(xsend.at[p], xbuf.at[me], xs.at[i], xr.at[me], p, tp).wait_send()
        remote(pbuf.at[p], rbuf.at[me], ps.at[i], pr.at[me], p, tp).wait_send()

    loop(1, n, sent)


def delta_kernel(
    keys, rows, scalars_ref, kq_ref, value_ref, state_ref, new_ref, read_ref, held
):
    g = pl.program_id(0)
    heads = state_ref.shape[1]
    key_dim, value_dim = state_ref.shape[2], state_ref.shape[3]
    turned = pltpu.roll(kq_ref[...], lax.rem(128 - STEP * g, 128), 1)
    values = pltpu.roll(value_ref[...], lax.rem(rows - STEP * g, rows), 0)
    for i in range(STEP):
        s = STEP * g + i
        for j in range(keys):
            q = jnp.broadcast_to(
                turned[:, j * rows + i : j * rows + i + 1], (key_dim, value_dim)
            )
            at = (keys + j) * rows + i
            k = jnp.broadcast_to(turned[:, at : at + 1], (key_dim, value_dim))
            qk = scalars_ref[s, 2 * heads + j]
            for h in range(j * (heads // keys), (j + 1) * (heads // keys)):
                cols = slice(h * value_dim, (h + 1) * value_dim)
                retain, strength = scalars_ref[s, h], scalars_ref[s, heads + h]
                decayed = state_ref[i, h] * retain
                predicted = jnp.sum(decayed * k, axis=0, keepdims=True)
                before = jnp.sum(decayed * q, axis=0, keepdims=True)
                correction = strength * (values[i : i + 1, cols] - predicted)
                new_ref[i, h] = decayed + k * correction
                held[i : i + 1, cols] = before + qk * correction
    row = lax.broadcasted_iota(jnp.int32, held.shape, 0)
    mine = (row >= STEP * g) & (row < STEP * (g + 1))
    read_ref[...] = jnp.where(mine, pltpu.roll(held[...], STEP * g, 0), read_ref[...])


def mix_kernel(
    n,
    m,
    read_ref,
    gate_ref,
    head_gain_ref,
    tokens_ref,
    ow_ref,
    ffn_gain_ref,
    eg_ref,
    eu_ref,
    ed_ref,
    sg_ref,
    su_ref,
    sd_ref,
    branch_ref,
    route_ref,
    out_ref,
    ow,
    eg,
    eu,
    ed,
    hbuf,
    mbuf,
    mrecv,
    ssend,
    sbuf,
    sdown,
    resid,
    fbuf,
    pbuf,
    srecv,
    rsend,
    rrecv,
    obuf,
    wsem,
    hs,
    hr,
    ms,
    mr,
    ss,
    sr,
    fs,
    fr,
    gs,
    gr,
    bs,
    br,
    rs,
    rr,
    os_,
    or_,
):
    me, tp = lax.axis_index("ep"), lax.axis_index("tp")
    count = n * m
    lin = me * m + tp
    half = m // 2
    core = lax.rem(tp, 2)
    pair = tp + 1 - 2 * core
    rows, width = tokens_ref.shape
    fetches = []
    split = width // 2
    moves = [(ow_ref, ow), (eg_ref, eg), (eu_ref, eu)]
    moves += [(ed_ref.at[0, :, pl.ds(c * split, split)], ed.at[c]) for c in range(2)]
    for i, (w, v) in enumerate(moves):
        c = pltpu.make_async_copy(w, v, wsem.at[i])
        c.start()
        fetches.append(c)

    barrier = pltpu.get_barrier_semaphore()

    def greet(i):
        p = lax.rem(lin + i, count)
        pl.semaphore_signal(
            barrier, inc=1, device_id=(p // m, lax.rem(p, m)), device_id_type=MESH
        )

    loop(1, count, greet)

    value_dim = head_gain_ref.shape[0]
    for h in range(0, read_ref.shape[1], value_dim):
        cols = slice(h, h + value_dim)
        hbuf[me, :, cols] = (
            rms_scale(read_ref[:, cols], head_gain_ref[...]) * gate_ref[:, cols]
        ).astype(BF16)
    pl.semaphore_wait(barrier, count - 1)

    def send_h(i):
        p = lax.rem(me + i, n)
        remote(hbuf.at[me], hbuf.at[me], hs.at[i], hr.at[me], p, tp).start()

    loop(1, n, send_h)
    units = ssend.shape[1] // 3
    for at, w in enumerate((sg_ref, su_ref, sd_ref)):
        by_unit = w[...] if at == 2 else w[...].astype(F32).T.astype(BF16)
        for e in range(n):
            ssend[e, at * units : (at + 1) * units] = by_unit[e * units : (e + 1) * units]
    fetches[0].wait()

    def got_h(i):
        p = lax.rem(me + i, n)
        remote(hbuf.at[p], hbuf.at[p], hs.at[i], hr.at[p], p, tp).wait_recv()

    loop(1, n, got_h)
    h_all = hbuf[...].reshape(n * rows, hbuf.shape[2])
    block = ow.shape[1]
    mbuf[...] = (
        jnp.dot(h_all, ow[...], preferred_element_type=F32).astype(BF16).reshape(n, rows, block)
    )

    def send_m(i):
        p = lax.rem(lin + i, count)
        e, t = p // m, lax.rem(p, m)
        remote(mbuf.at[e], mrecv.at[lin], ms.at[i], mr.at[lin], e, t).start()

    loop(1, count, send_m)
    mrecv[lin] = mbuf[me]

    def send_s(i):
        p = lax.rem(me + i, n)
        remote(ssend.at[p], sbuf.at[me], ss.at[i], sr.at[me], p, tp).start()

    loop(1, n, send_s)
    sbuf[me] = ssend[me]

    def got_m(i):
        p = lax.rem(lin + i, count)
        e, t = p // m, lax.rem(p, m)
        remote(mrecv.at[p], mrecv.at[p], ms.at[i], mr.at[p], e, t).wait_recv()

    loop(1, count, got_m)
    pieces = []
    for e in range(n):
        acc = mrecv[e * m].astype(F32)
        for t in range(1, m):
            acc = acc + mrecv[e * m + t].astype(F32)
        pieces.append(acc)
    mix = jnp.concatenate(pieces, axis=1)
    residual = (tokens_ref[...].astype(F32) + mix).astype(BF16).astype(F32)
    quarter = width // m
    for t in range(m):
        resid[t] = residual[:, t * quarter : (t + 1) * quarter]
    ffn_in = rms_scale(residual, ffn_gain_ref[...]).astype(BF16)
    fbuf[0, me] = ffn_in[:, :split]
    fbuf[1, me] = ffn_in[:, split:]

    def send_f(i):
        p = lax.rem(me + i, n)
        remote(
            fbuf.at[core, me], fbuf.at[core, me], fs.at[i], fr.at[core, me], p, tp
        ).start()

    loop(1, n, send_f)

    def pass_f(i):
        p = lax.rem(me + n - i, n)
        mine = fbuf.at[core, p]
        remote(mine, mine, fs.at[i], fr.at[core, p], p, tp).wait_recv()
        remote(mine, mine, gs.at[i], gr.at[p], me, pair).start()

    loop(1, n, pass_f)

    def got_s(i):
        p = lax.rem(me + i, n)
        remote(sbuf.at[p], sbuf.at[p], ss.at[i], sr.at[p], p, tp).wait_recv()

    loop(1, n, got_s)
    shared = jnp.concatenate([sbuf[e] for e in range(n)], axis=1)
    for c in range(2):
        sdown[c] = shared[2 * units :, c * split : (c + 1) * split]
    for c in fetches[1:]:
        c.wait()

    def got_f(i):
        p = lax.rem(me + n - i, n)
        other = fbuf.at[1 - core, p]
        remote(other, other, gs.at[i], gr.at[p], me, pair).wait_recv()

    loop(1, n, got_f)

    x0 = fbuf[0].reshape(n * rows, split)
    x1 = fbuf[1].reshape(n * rows, split)

    def up(w):
        return jnp.dot(x0, w[0, :split], preferred_element_type=F32) + jnp.dot(
            x1, w[0, split:], preferred_element_type=F32
        )

    def up_shared(w):
        return dot_nt(x0, w[:, :split]) + dot_nt(x1, w[:, split:])

    act = (silu(up(eg)) * up(eu)).astype(BF16)
    shared_act = (
        silu(up_shared(shared[:units])) * up_shared(shared[units : 2 * units])
    ).astype(BF16)
    bg = branch_ref[...].astype(F32).reshape(1, -1)
    branch = sigmoid(
        jnp.sum(x0.astype(F32) * bg[:, :split], axis=1, keepdims=True)
        + jnp.sum(x1.astype(F32) * bg[:, split:], axis=1, keepdims=True)
    )
    weight = route_ref[:, 0:1]

    def down(c):
        out = weight * jnp.dot(act, ed[c], preferred_element_type=F32)
        out = out + branch * jnp.dot(shared_act, sdown[c], preferred_element_type=F32)
        pbuf[c] = out.astype(BF16)

    down(1 - core)
    swap = remote(pbuf.at[1 - core], srecv, bs.at[0], br.at[0], me, pair)
    swap.start()
    down(core)
    swap.wait_recv()
    for e in range(n):
        these = slice(e * rows, (e + 1) * rows)
        both = pbuf[core, these].astype(F32) + srecv[these].astype(F32)
        for x in range(half):
            rsend[e * half + x] = both[:, x * quarter : (x + 1) * quarter].astype(BF16)

    blocks = n * half
    mine = me * half + tp // 2

    def send_r(i):
        p = lax.rem(mine + i, blocks)
        e, x = p // half, lax.rem(p, half)
        remote(rsend.at[p], rrecv.at[mine], rs.at[i], rr.at[mine], e, 2 * x + core).start()

    loop(1, blocks, send_r)
    rrecv[mine] = rsend[mine]

    def got_r(i):
        p = lax.rem(mine + i, blocks)
        e, x = p // half, lax.rem(p, half)
        remote(rrecv.at[p], rrecv.at[p], rs.at[i], rr.at[p], e, 2 * x + core).wait_recv()

    loop(1, blocks, got_r)
    place = core * half + tp // 2
    acc = resid[place]
    for p in range(blocks):
        acc = acc + rrecv[p].astype(F32)
    obuf[place] = acc.astype(BF16)

    def send_o(i):
        t = lax.rem(tp + i, m)
        remote(obuf.at[place], obuf.at[place], os_.at[i], or_.at[place], me, t).start()

    loop(1, m, send_o)

    def got_o(i):
        t = lax.rem(tp + i, m)
        there = lax.rem(t, 2) * half + t // 2
        remote(obuf.at[there], obuf.at[there], os_.at[i], or_.at[there], me, t).wait_recv()

    loop(1, m, got_o)
    for t in range(m):
        out_ref[:, t * quarter : (t + 1) * quarter] = obuf[t]

    def sent_ep(i):
        p = lax.rem(me + i, n)
        remote(hbuf.at[me], hbuf.at[me], hs.at[i], hr.at[me], p, tp).wait_send()
        remote(ssend.at[p], sbuf.at[me], ss.at[i], sr.at[me], p, tp).wait_send()
        remote(
            fbuf.at[core, me], fbuf.at[core, me], fs.at[i], fr.at[core, me], p, tp
        ).wait_send()
        b = lax.rem(me + n - i, n)
        remote(fbuf.at[core, b], fbuf.at[core, b], gs.at[i], gr.at[b], me, pair).wait_send()

    loop(1, n, sent_ep)

    def sent_m(i):
        p = lax.rem(lin + i, count)
        e, t = p // m, lax.rem(p, m)
        remote(mbuf.at[e], mrecv.at[lin], ms.at[i], mr.at[lin], e, t).wait_send()

    loop(1, count, sent_m)
    swap.wait_send()

    def sent_r(i):
        p = lax.rem(mine + i, blocks)
        e, x = p // half, lax.rem(p, half)
        remote(
            rsend.at[p], rrecv.at[mine], rs.at[i], rr.at[mine], e, 2 * x + core
        ).wait_send()

    loop(1, blocks, sent_r)

    def sent_o(i):
        t = lax.rem(tp + i, m)
        remote(obuf.at[place], obuf.at[place], os_.at[i], or_.at[place], me, t).wait_send()

    loop(1, m, sent_o)


VMEM = pl.BlockSpec(memory_space=pltpu.VMEM)
ANY = pl.BlockSpec(memory_space=pl.ANY)


def per_device(
    n,
    m,
    tokens,
    norm_gain,
    query_weight,
    key_weight,
    value_weight,
    outgate_weight,
    beta_weight,
    decay_weight,
    decay_rate,
    decay_bias,
    head_gain,
    recurrent,
    output_weight,
    ffn_gain,
    routes,
    route_weight,
    expert_gate,
    expert_up,
    expert_down,
    shared_gate,
    shared_up,
    shared_down,
    branch_gate,
):
    rows, width = tokens.shape
    _, heads, key_dim, value_dim = recurrent.shape
    depth, qc = query_weight.shape
    vc = value_weight.shape[1]
    keys = qc // key_dim
    total = 2 * qc + 2 * vc
    sds = jax.ShapeDtypeStruct
    dma = pltpu.SemaphoreType.DMA
    units = shared_gate.shape[1] // n
    cols = shared_down.shape[1]
    kq, value, gate, scalars, route = pl.pallas_call(
        functools.partial(project_kernel, n, key_dim),
        out_shape=(
            sds((key_dim, 128), F32),
            sds((rows, vc), F32),
            sds((rows, vc), F32),
            sds((rows, 2 * heads + keys), F32),
            sds((n * rows, 128), F32),
        ),
        in_specs=[VMEM] * 2 + [ANY] * 4 + [VMEM] * 6,
        out_specs=(VMEM,) * 5,
        scratch_shapes=[
            pltpu.VMEM((depth, total), BF16),
            pltpu.VMEM((n, rows, depth), BF16),
            pltpu.VMEM((n, rows, depth), BF16),
            pltpu.VMEM((n, rows, total + 128), BF16),
            pltpu.VMEM((n, rows, total + 128), BF16),
            dma((4,)),
            dma((n,)),
            dma((n,)),
            dma((n,)),
            dma((n,)),
        ],
        compiler_params=pltpu.CompilerParams(collective_id=0, has_side_effects=True),
    )(
        tokens,
        norm_gain,
        query_weight,
        key_weight,
        value_weight,
        outgate_weight,
        beta_weight.T,
        decay_weight.T,
        decay_rate[None, :],
        decay_bias[None, :],
        routes.T,
        route_weight.T,
    )

    new_state, readout = pl.pallas_call(
        functools.partial(delta_kernel, keys, rows),
        out_shape=(sds(recurrent.shape, F32), sds((rows, vc), F32)),
        grid=(rows // STEP,),
        in_specs=[
            pl.BlockSpec(memory_space=pltpu.SMEM),
            pl.BlockSpec((key_dim, 128), lambda g: (0, 0)),
            pl.BlockSpec((rows, vc), lambda g: (0, 0)),
            pl.BlockSpec((STEP, heads, key_dim, value_dim), lambda g: (g, 0, 0, 0)),
        ],
        out_specs=(
            pl.BlockSpec((STEP, heads, key_dim, value_dim), lambda g: (g, 0, 0, 0)),
            pl.BlockSpec((rows, vc), lambda g: (0, 0)),
        ),
        scratch_shapes=[pltpu.VMEM((rows, vc), F32)],
        compiler_params=pltpu.CompilerParams(dimension_semantics=("arbitrary",)),
    )(scalars, kq, value, recurrent)

    quarter = width // m
    blocks = n * (m // 2)
    layer_out = pl.pallas_call(
        functools.partial(mix_kernel, n, m),
        out_shape=sds((rows, width), BF16),
        in_specs=[VMEM] * 4 + [ANY, VMEM] + [ANY] * 3 + [VMEM] * 5,
        out_specs=VMEM,
        scratch_shapes=[
            pltpu.VMEM(output_weight.shape, BF16),
            pltpu.VMEM(expert_gate.shape, BF16),
            pltpu.VMEM(expert_up.shape, BF16),
            pltpu.VMEM((2, expert_down.shape[1], width // 2), BF16),
            pltpu.VMEM((n, rows, vc), BF16),
            pltpu.VMEM((n, rows, cols), BF16),
            pltpu.VMEM((n * m, rows, cols), BF16),
            pltpu.VMEM((n, 3 * units, cols), BF16),
            pltpu.VMEM((n, 3 * units, cols), BF16),
            pltpu.VMEM((2, units, width // 2), BF16),
            pltpu.VMEM((m, rows, quarter), F32),
            pltpu.VMEM((2, n, rows, width // 2), BF16),
            pltpu.VMEM((2, n * rows, width // 2), BF16),
            pltpu.VMEM((n * rows, width // 2), BF16),
            pltpu.VMEM((blocks, rows, quarter), BF16),
            pltpu.VMEM((blocks, rows, quarter), BF16),
            pltpu.VMEM((m, rows, quarter), BF16),
            dma((5,)),
            dma((n,)),
            dma((n,)),
            dma((n * m,)),
            dma((n * m,)),
            dma((n,)),
            dma((n,)),
            dma((n,)),
            dma((2, n)),
            dma((n,)),
            dma((n,)),
            dma((1,)),
            dma((1,)),
            dma((blocks,)),
            dma((blocks,)),
            dma((m,)),
            dma((m,)),
        ],
        compiler_params=pltpu.CompilerParams(collective_id=1, has_side_effects=True),
    )(
        readout,
        gate,
        head_gain,
        tokens,
        output_weight,
        ffn_gain,
        expert_gate,
        expert_up,
        expert_down,
        shared_gate,
        shared_up,
        shared_down,
        branch_gate,
        route,
    )
    return (layer_out, new_state)


def solution(mesh):
    return jax.shard_map(
        functools.partial(per_device, mesh.shape["ep"], mesh.shape["tp"]),
        mesh=mesh,
        in_specs=(
            P("ep", None),
            P(),
            P("ep", "tp"),
            P("ep", "tp"),
            P("ep", "tp"),
            P("ep", "tp"),
            P(),
            P(),
            P("tp"),
            P("tp"),
            P(),
            P("ep", "tp", None, None),
            P("tp", "ep"),
            P(),
            P("ep", None),
            P("ep", None),
            P("ep", None, "tp"),
            P("ep", None, "tp"),
            P("ep", "tp", None),
            P("ep", "tp"),
            P("ep", "tp"),
            P("tp", "ep"),
            P(),
        ),
        out_specs=(P("ep", None), P("ep", "tp", None, None)),
        check_vma=False,
    )
```
